32 devices in a mesh: sp: 8 (over z, x), tp: 4 (over y, core).
Axes of the slice: x: 2, y: 2, z: 4, core: 2. Of those that a mesh axis runs over, the one named last changes fastest.
Arguments:
- inputs: bfloat16 [3072, 4096], P('sp', 'tp'), may hold values from -40 to 40, as said below
- query_weight: bfloat16 [2, 4096, 1024], P(None, None, 'tp'), may hold values from -0.2 to 0.2
- key_weight: bfloat16 [2, 4096, 1024], P(None, None, 'tp'), may hold values from -0.2 to 0.2
- value_weight: bfloat16 [4096, 2048], P(None, 'tp'), may hold values from -0.09375 to 0.09375
- pool_weight: bfloat16 [4096, 2048], P(None, 'tp'), may hold values from -0.09375 to 0.09375
- mix_lambda: float32 [16], P('tp'), may hold values from 0.3 to 0.8
- head_gain: float32 [128], replicated, may hold values from 0.1 to 1.9
- attn_out_weight: bfloat16 [2048, 4096], P('tp'), may hold values from -0.125 to 0.125
- pool_out_weight: bfloat16 [2048, 4096], P('tp'), may hold values from -0.125 to 0.125
Outputs:
- mixed: bfloat16 [3072, 4096], P(('sp', 'tp'))
- log_totals: float32 [2, 16, 3072], P(None, 'tp', 'sp')
The draws below stay inside these ranges and needn't reach their ends.
Inputs may be any that keep to these rules, and one draw needn't show every extreme that they name: inputs of order one, in some draws a few rows larger.
All inputs are finite; a program needn't handle non-finite values.
Results may differ from the reference program's by a relative error of at most 0.015.
Values may be sent and summed in bfloat16 or wider, within the bound.
No kernel may reach another device: no remote copies, remote signals or barrier semaphores. Data moves between devices by JAX's collectives and lax.ppermute only.
A program may use at most 192 MiB of HBM per device.

```python
import jax
import jax.numpy as jnp
from jax import lax

D = 4096
HEADS = 16
HEAD_DIM = 64
POOL_WIDTH = 2048
TOK_DEV = 384
TOKENS = 3072
N_TP = 4


def shared_query(key):
    return jax.random.normal(jax.random.fold_in(key, 101), (2, D, HEADS * HEAD_DIM), jnp.float32) * (1.32 * D ** (-0.5))


def draw_query_weight(key, part):
    return jnp.clip(shared_query(key), -0.199, 0.199).astype(jnp.bfloat16)


def draw_key_weight(key, part):
    own = jax.random.normal(jax.random.fold_in(key, 202), (2, D, HEADS * HEAD_DIM), jnp.float32) * (1.32 * D ** (-0.5))
    return jnp.clip(own, -0.199, 0.199).astype(jnp.bfloat16)


def draw_inputs(key, part):
    base = jnp.clip(jax.random.normal(jax.random.fold_in(key, 303), (TOKENS, D), jnp.float32), -6.0, 6.0)
    return jnp.clip(base, -40.0, 40.0).astype(jnp.bfloat16)


def level_of(key, shape, cuts, smallest, high):
    level, own = 1.0, jax.random.fold_in(key, 6)
    for axis_at, shards_of in cuts:
        heights = jnp.exp(jax.random.uniform(jax.random.fold_in(own, axis_at), (shards_of,), jnp.float32, smallest / len(cuts), high / len(cuts)))
        level = level * jnp.repeat(heights, shape[axis_at] // shards_of).reshape([-1 if axis == axis_at else 1 for axis in range(len(shape))])
    return level


def bell_draw(rng, extent, deviation, most, shards=(), kind=jnp.bfloat16):
    array = jax.random.normal(rng, extent, jnp.float32) * deviation
    if len(shards) > 0:
        array = level_of(rng, extent, shards, -0.22, 0.18) * array
    return jnp.clip(array, min=-most, max=most).astype(kind)


def setup_inputs(seed: int = 0) -> dict:
    seeds = jax.random.split(jax.random.key(seed), 10)
    inputs = draw_inputs(jax.random.fold_in(seeds[9], 71), 0)
    query_weight = draw_query_weight(jax.random.fold_in(seeds[9], 71), 0)
    key_weight = draw_key_weight(jax.random.fold_in(seeds[9], 71), 0)
    value_weight = bell_draw(seeds[3], (D, HEADS * 2 * HEAD_DIM), D ** -0.5, 0.09375, ((1, 4),))
    pool_weight = bell_draw(seeds[4], (D, POOL_WIDTH), D ** -0.5, 0.09375, ((1, 4),))
    mix_lambda = jnp.clip(0.3 + 0.5 * jax.random.uniform(seeds[5], (HEADS,), jnp.float32) ** level_of(seeds[5], (HEADS,), ((0, 4),), -0.2, 0.2), 0.3, 0.8)
    head_gain = jnp.clip(1.0 + 0.18 * jax.random.normal(seeds[6], (2 * HEAD_DIM,), jnp.float32), 0.1, 1.9)
    attn_out_weight = bell_draw(seeds[7], (HEADS * 2 * HEAD_DIM, D), (HEADS * 2 * HEAD_DIM) ** -0.5, 0.125, ((0, 4),))
    pool_out_weight = bell_draw(seeds[8], (POOL_WIDTH, D), POOL_WIDTH ** -0.5, 0.125, ((0, 4),))
    return dict(inputs=inputs, query_weight=query_weight, key_weight=key_weight, value_weight=value_weight, pool_weight=pool_weight, mix_lambda=mix_lambda, head_gain=head_gain, attn_out_weight=attn_out_weight, pool_out_weight=pool_out_weight)


def head_block(query_rows, key_rows, value_rows, lam_value, head_gain):
    scores = jnp.einsum('mqd,mkd->mqk', query_rows.astype(jnp.float32), key_rows.astype(jnp.float32)) * HEAD_DIM ** (-0.5)
    row_max = lax.optimization_barrier(jnp.max(scores, axis=-1))
    expo = jnp.exp(scores - row_max[..., None])
    totals = lax.optimization_barrier(jnp.sum(expo, axis=-1))
    weights = expo.astype(jnp.bfloat16).astype(jnp.float32)
    numer = jnp.einsum('mqk,ke->mqe', weights, value_rows.astype(jnp.float32))
    diff = numer[0] / totals[0][:, None] - lam_value * numer[1] / totals[1][:, None]
    scaled = diff * lax.rsqrt(lax.optimization_barrier(jnp.mean(diff * diff, axis=-1, keepdims=True)) + 1e-05) * head_gain
    return (scaled.astype(jnp.bfloat16), row_max + jnp.log(totals))

def reference(inputs, query_weight, key_weight, value_weight, pool_weight, mix_lambda, head_gain, attn_out_weight, pool_out_weight):
    total_tok = inputs.shape[0]
    queries = jnp.stack([jnp.dot(inputs, query_weight[m], preferred_element_type=jnp.float32) for m in range(2)]).astype(jnp.bfloat16)
    keys = jnp.stack([jnp.dot(inputs, key_weight[m], preferred_element_type=jnp.float32) for m in range(2)]).astype(jnp.bfloat16)
    values = jnp.dot(inputs, value_weight, preferred_element_type=jnp.float32).astype(jnp.bfloat16)
    pool_in = jnp.dot(inputs, pool_weight, preferred_element_type=jnp.float32).astype(jnp.bfloat16)
    query_heads = queries.reshape(2, total_tok, HEADS, HEAD_DIM).transpose(2, 0, 1, 3)
    key_heads = keys.reshape(2, total_tok, HEADS, HEAD_DIM).transpose(2, 0, 1, 3)
    value_heads = values.reshape(total_tok, HEADS, 2 * HEAD_DIM).transpose(1, 0, 2)
    blocks = total_tok // TOK_DEV

    def one_head(packed):
        query_rows, key_rows, value_rows, lam_value = packed
        query_blocks = query_rows.reshape(2, blocks, TOK_DEV, HEAD_DIM).transpose(1, 0, 2, 3)
        outs, logs = lax.map(lambda block: head_block(block, key_rows, value_rows, lam_value, head_gain), query_blocks)
        return (outs.reshape(total_tok, 2 * HEAD_DIM), logs.transpose(1, 0, 2).reshape(2, total_tok))
    head_outs, head_logs = lax.map(one_head, (query_heads, key_heads, value_heads, mix_lambda))
    attn = head_outs.transpose(1, 0, 2).reshape(total_tok, HEADS * 2 * HEAD_DIM)
    log_totals = head_logs.transpose(1, 0, 2)
    pool_f = pool_in.astype(jnp.float32)
    padded = jnp.pad(pool_f, ((8, 8), (0, 0)))
    position = jnp.arange(total_tok, dtype=jnp.int32)
    group_width = POOL_WIDTH // 4
    pieces = []
    for group_index, reach in enumerate((2, 4, 8, 16)):
        radius = reach // 2
        cols = slice(group_index * group_width, (group_index + 1) * group_width)
        window_sum = padded[8 - radius:8 - radius + total_tok, cols]
        for shift_by in range(-radius + 1, radius):
            window_sum = window_sum + padded[8 + shift_by:8 + shift_by + total_tok, cols]
        low = jnp.clip(position - radius, 0, total_tok)
        high = jnp.clip(position + radius, 0, total_tok)
        pieces.append(window_sum / (high - low).astype(jnp.float32)[:, None] - pool_f[:, cols])
    pooled = jnp.concatenate(pieces, axis=1).astype(jnp.bfloat16)
    attn_cols = HEADS * 2 * HEAD_DIM // N_TP
    pool_cols = POOL_WIDTH // N_TP
    summed = jnp.zeros((total_tok, D), jnp.float32)
    for group_index in range(N_TP):
        a_cols = slice(group_index * attn_cols, (group_index + 1) * attn_cols)
        p_cols = slice(group_index * pool_cols, (group_index + 1) * pool_cols)
        partial_value = jnp.dot(attn[:, a_cols], attn_out_weight[a_cols], preferred_element_type=jnp.float32)
        partial_value = partial_value + jnp.dot(pooled[:, p_cols], pool_out_weight[p_cols], preferred_element_type=jnp.float32)
        rounded = lax.optimization_barrier(partial_value.astype(jnp.bfloat16))
        summed = summed + rounded.astype(jnp.float32)
    return (summed.astype(jnp.bfloat16), log_totals)
```

```python
import functools

import jax
import jax.numpy as jnp
from jax import lax
from jax.experimental import pallas as pl
from jax.experimental.pallas import tpu as pltpu
from jax.sharding import PartitionSpec as P

HEAD_DIM = 64
POOL_WIDTH = 2048
F32 = jnp.float32
BF16 = jnp.bfloat16


def swap(value, axis, offset):
    count = lax.axis_size(axis)
    return lax.ppermute(value, axis, [(i, i ^ offset) for i in range(count)])


def project(pieces, blocks, weights, kind, first, rank):
    rows, depth = pieces[0].shape
    count = len(pieces)
    shaped, plain = weights
    half = shaped.shape[2]
    heads = half // HEAD_DIM
    wide = plain.shape[1]
    steps = 2
    sub = depth // steps
    acc_shape = jax.ShapeDtypeStruct((rows, 2 * half + wide), F32)

    def body(scalars, *refs):
        x_refs, refs = refs[:count], refs[count:]
        s_refs, refs = refs[:count], refs[count:]
        p_refs, refs = refs[:count], refs[count:]
        if first is not None:
            init, refs = refs[0], refs[1:]
        outs, acc = refs[:-1], refs[-1]
        step = pl.program_id(0)

        @pl.when(step == 0)
        def _():
            if first is not None:
                acc[...] = init[...]
            else:
                acc[...] = jnp.zeros_like(acc)

        for m in range(2):
            total = acc[:, m * half : (m + 1) * half]
            for x_ref, s_ref in zip(x_refs, s_refs):
                total = total + jnp.dot(x_ref[...], s_ref[m], preferred_element_type=F32)
            acc[:, m * half : (m + 1) * half] = total
        total = acc[:, 2 * half :]
        for x_ref, p_ref in zip(x_refs, p_refs):
            total = total + jnp.dot(x_ref[...], p_ref[...], preferred_element_type=F32)
        acc[:, 2 * half :] = total

        @pl.when(step == steps - 1)
        def _():
            if kind is None:
                outs[0][...] = acc[...]
                return
            lead = scalars[count]
            narrow = 4 * HEAD_DIM if kind == "kv" else 2 * HEAD_DIM
            hold = outs[-1]
            for h in range(heads):
                cols = [acc[:, m * half + h * HEAD_DIM : m * half + (h + 1) * HEAD_DIM] for m in range(2)]
                if kind == "kv":
                    start = 2 * half + h * 2 * HEAD_DIM
                    cols.append(acc[:, start : start + 2 * HEAD_DIM])
                hold[h ^ lead] = jnp.concatenate(cols, axis=1).astype(BF16)
            if kind == "qp":
                outs[-2][...] = acc[:, 2 * half :].astype(BF16)

    def w_shaped(i):
        return pl.BlockSpec((2, sub, half), lambda k, sc: (0, sc[i] * steps + k, 0))

    def w_plain(i):
        return pl.BlockSpec((sub, wide), lambda k, sc: (sc[i] * steps + k, 0))

    in_specs = [pl.BlockSpec((rows, sub), lambda k, sc: (0, k)) for _ in range(count)]
    in_specs += [w_shaped(i) for i in range(count)] + [w_plain(i) for i in range(count)]
    args = list(pieces) + [shaped] * count + [plain] * count
    if first is not None:
        in_specs.append(pl.BlockSpec(acc_shape.shape, lambda k, sc: (0, 0)))
        args.append(first)
    if kind is None:
        out_shape = [acc_shape]
    else:
        narrow = 4 * HEAD_DIM if kind == "kv" else 2 * HEAD_DIM
        out_shape = []
        if kind == "qp":
            out_shape.append(jax.ShapeDtypeStruct((rows, wide), BF16))
        out_shape.append(jax.ShapeDtypeStruct((heads, rows, narrow), BF16))
    out_specs = [pl.BlockSpec(o.shape, lambda k, sc, n=len(o.shape): (0,) * n) for o in out_shape]
    scalars = jnp.stack([b.astype(jnp.int32) for b in blocks] + [rank.astype(jnp.int32)])
    return pl.pallas_call(
        body,
        grid_spec=pltpu.PrefetchScalarGridSpec(
            num_scalar_prefetch=1,
            grid=(steps,),
            in_specs=in_specs,
            out_specs=out_specs,
            scratch_shapes=[pltpu.VMEM(acc_shape.shape, F32)],
        ),
        out_shape=out_shape,
        compiler_params=pltpu.CompilerParams(vmem_limit_bytes=56 * 2**20),
        name="project",
    )(scalars, *args)


def attend(q, kv, state, lam, gain):
    blocks, rows, width = q.shape
    count = len(kv)
    last = state is not None

    def body(*refs):
        lam_ref, gain_ref, q_ref, refs = refs[0], refs[1], refs[2], refs[3:]
        kv_refs, refs = refs[:count], refs[count:]
        if last:
            acc_in, max_in, attn_ref, log_ref = refs
        else:
            acc_out, max_out = refs
        query = q_ref[0] * jnp.asarray(HEAD_DIM ** (-0.5), BF16)
        lane = lax.broadcasted_iota(jnp.int32, (rows, width), 1)
        ones = jnp.ones((kv_refs[0].shape[0], 2 * HEAD_DIM), BF16)
        maps = []
        for m in range(2):
            mine = (lane // HEAD_DIM) == m
            query_m = jnp.where(mine, query, jnp.zeros_like(query))
            scores = [
                lax.dot_general(
                    query_m, r[:, : 2 * HEAD_DIM], (((1,), (1,)), ((), ())), preferred_element_type=F32
                )
                for r in kv_refs
            ]
            top = scores[0]
            for s in scores[1:]:
                top = jnp.maximum(top, s)
            top = jnp.max(top, axis=1, keepdims=True)
            if last:
                old = max_in[0, m][:, :1]
                top = jnp.maximum(top, old)
                total = acc_in[0, m] * jnp.exp(old - top)
            else:
                total = None
            for s, r in zip(scores, kv_refs):
                expo = jnp.exp(s - top).astype(BF16)
                side = jnp.concatenate([r[:, 2 * HEAD_DIM :], ones], axis=1)
                add = jnp.dot(expo, side, preferred_element_type=F32)
                total = add if total is None else total + add
            if not last:
                acc_out[0, m] = total
                max_out[0, m] = jnp.broadcast_to(top, (rows, 2 * HEAD_DIM))
            else:
                sums = total[:, 2 * HEAD_DIM :]
                maps.append(total[:, : 2 * HEAD_DIM] / sums)
                log_ref[0, m : m + 1, :] = jnp.transpose(top + jnp.log(sums))[:1]
        if last:
            diff = maps[0] - lam_ref[0] * maps[1]
            norm = lax.rsqrt(jnp.mean(diff * diff, axis=1, keepdims=True) + 1e-05)
            attn_ref[0] = (diff * norm * gain_ref[...]).astype(BF16)

    whole = 4 * HEAD_DIM
    in_specs = [
        pl.BlockSpec(memory_space=pltpu.SMEM),
        pl.BlockSpec((1, gain.shape[1]), lambda b: (0, 0)),
        pl.BlockSpec((1, rows, width), lambda b: (b, 0, 0)),
    ] + [pl.BlockSpec(a.shape, lambda b: (0, 0)) for a in kv]
    acc_spec = pl.BlockSpec((1, 2, rows, whole), lambda b: (b, 0, 0, 0))
    max_spec = pl.BlockSpec((1, 2, rows, 2 * HEAD_DIM), lambda b: (b, 0, 0, 0))
    args = [lam, gain, q, *kv]
    if last:
        in_specs += [acc_spec, max_spec]
        args += list(state)
        out_shape = [
            jax.ShapeDtypeStruct((blocks, rows, 2 * HEAD_DIM), BF16),
            jax.ShapeDtypeStruct((blocks, 2, rows), F32),
        ]
        out_specs = [
            pl.BlockSpec((1, rows, 2 * HEAD_DIM), lambda b: (b, 0, 0)),
            pl.BlockSpec((1, 2, rows), lambda b: (b, 0, 0)),
        ]
    else:
        out_shape = [
            jax.ShapeDtypeStruct((blocks, 2, rows, whole), F32),
            jax.ShapeDtypeStruct((blocks, 2, rows, 2 * HEAD_DIM), F32),
        ]
        out_specs = [acc_spec, max_spec]
    pairs = 2 * blocks * rows * count * kv[0].shape[0]
    return pl.pallas_call(
        body,
        grid=(blocks,),
        in_specs=in_specs,
        out_specs=out_specs,
        out_shape=out_shape,
        cost_estimate=pl.CostEstimate(flops=pairs * 12 * HEAD_DIM, bytes_accessed=8 << 20, transcendentals=pairs),
        compiler_params=pltpu.CompilerParams(vmem_limit_bytes=56 * 2**20),
        name="attend",
    )(*args)


def pool(pool_in, before, after):
    tok_rows, channels = pool_in.shape
    padded = jnp.concatenate([before, pool_in, after], axis=0).astype(F32)
    total_tok = tok_rows * lax.axis_size("sp")
    position = lax.axis_index("sp") * tok_rows + jnp.arange(tok_rows, dtype=jnp.int32)
    group = (lax.axis_index("tp") * channels + jnp.arange(channels, dtype=jnp.int32)) // (POOL_WIDTH // 4)
    result = jnp.zeros((tok_rows, channels), F32)
    for group_index, reach in enumerate((2, 4, 8, 16)):
        radius = reach // 2
        window_sum = padded[8 - radius : 8 - radius + tok_rows]
        for shift_by in range(-radius + 1, radius):
            window_sum = window_sum + padded[8 + shift_by : 8 + shift_by + tok_rows]
        low = jnp.clip(position - radius, 0, total_tok)
        high = jnp.clip(position + radius, 0, total_tok)
        window_mean = window_sum / (high - low).astype(F32)[:, None]
        result = jnp.where((group == group_index)[None, :], window_mean, result)
    return (result - pool_in.astype(F32)).astype(BF16)


def on_device(
    inputs,
    query_weight,
    key_weight,
    value_weight,
    pool_weight,
    mix_lambda,
    head_gain,
    attn_out_weight,
    pool_out_weight,
):
    tok_rows = inputs.shape[0]
    heads = query_weight.shape[2] // HEAD_DIM
    n_sp, n_tp = lax.axis_size("sp"), lax.axis_size("tp")
    sp, tp = lax.axis_index("sp"), lax.axis_index("tp")
    rank = sp % heads

    pieces = {0: inputs}
    for offset in range(2, n_tp, 2):
        pieces[offset] = swap(inputs, "tp", offset)
    pieces[1] = swap(inputs, "tp", 1)
    near, far = [0, 1], list(range(2, n_tp))
    place = lambda which: ([pieces[d] for d in which], [tp ^ d for d in which])
    kv_weights, qp_weights = (key_weight, value_weight), (query_weight, pool_weight)
    (kv_sum,) = project(*place(near), kv_weights, None, None, rank)
    (qp_sum,) = project(*place(near), qp_weights, None, None, rank)
    for offset in range(2, n_tp, 2):
        pieces[offset + 1] = swap(pieces[offset], "tp", 1)
    (kv,) = project(*place(far), kv_weights, "kv", kv_sum, rank)
    pool_in, q = project(*place(far), qp_weights, "qp", qp_sum, rank)

    kv_parts = [kv[0]] + [swap(kv[d % heads], "sp", d) for d in range(1, n_sp)]
    q_parts = [q[0]] + [swap(q[d], "sp", d) for d in range(1, heads)]
    up = [(i, i + 1) for i in range(n_sp - 1)]
    before = lax.ppermute(pool_in[tok_rows - 8 :], "sp", up)
    after = lax.ppermute(pool_in[:8], "sp", [(j, i) for i, j in up])
    pooled = pool(pool_in, before, after)

    lam = lax.dynamic_slice(mix_lambda, (rank,), (1,))
    gain = head_gain[None, :]
    queries = jnp.stack(q_parts)
    state = attend(queries, kv_parts[: n_sp // 2], None, lam, gain)
    attn, logs = attend(queries, kv_parts[n_sp // 2 :], state, lam, gain)

    mine = jnp.zeros((tok_rows, heads * 2 * HEAD_DIM), BF16)
    log_totals = jnp.zeros((2, heads, tok_rows), F32)
    for d in range(heads):
        part, log = attn[d], logs[d]
        if d:
            part, log = swap(part, "sp", d), swap(log, "sp", d)
        mine = lax.dynamic_update_slice(mine, part, (0, (rank ^ d) * 2 * HEAD_DIM))
        log_totals = lax.dynamic_update_slice(log_totals, log[:, None, :], (0, rank ^ d, 0))

    out_rows = tok_rows // n_tp

    def partial(d):
        at = (tp ^ d) * out_rows
        a = lax.dynamic_slice(mine, (at, 0), (out_rows, mine.shape[1]))
        p = lax.dynamic_slice(pooled, (at, 0), (out_rows, pooled.shape[1]))
        return (
            jnp.dot(a, attn_out_weight, preferred_element_type=F32)
            + jnp.dot(p, pool_out_weight, preferred_element_type=F32)
        ).astype(BF16)

    total = None
    for e in list(range(2, n_tp, 2)) + [0]:
        other = swap(partial(e + 1), "tp", 1)
        pair = partial(e).astype(F32) + other.astype(F32)
        if e:
            pair = swap(pair.astype(BF16), "tp", e).astype(F32)
        total = pair if total is None else total + pair
    return (total.astype(BF16), log_totals)


def solution(mesh):
    in_specs = (
        P("sp", "tp"),
        P(None, None, "tp"),
        P(None, None, "tp"),
        P(None, "tp"),
        P(None, "tp"),
        P("tp"),
        P(),
        P("tp", None),
        P("tp", None),
    )
    out_specs = (P(("sp", "tp"), None), P(None, "tp", "sp"))
    return jax.shard_map(
        on_device, mesh=mesh, in_specs=in_specs, out_specs=out_specs, check_vma=False
    )
```

```python
import jax
import jax.numpy as jnp
from jax import lax
from jax.experimental import pallas as pl
from jax.experimental.pallas import tpu as pltpu
from jax.sharding import PartitionSpec as P


HEAD_DIM = 64
POOL_WIDTH = 2048
F32 = jnp.float32
BF16 = jnp.bfloat16


LOG_TERMS = 3


def log_rows(rows):
    return -(-2 * LOG_TERMS * rows // (2 * HEAD_DIM) // 16) * 16


def swap(value, axis, offset):
    count = lax.axis_size(axis)
    return lax.ppermute(value, axis, [(i, i ^ offset) for i in range(count)])


def project(pieces, blocks, shaped, plain, first, rank):
    rows, depth = pieces[0].shape
    count, n_shaped = len(pieces), len(shaped)
    half = shaped[0].shape[2] if shaped else 0
    heads = half // HEAD_DIM
    wide = plain.shape[1]
    steps = 2
    sub = depth // steps
    pair = 2 * HEAD_DIM
    acc_shape = jax.ShapeDtypeStruct((rows, 2 * half * n_shaped + wide), F32)

    def body(scalars, *refs):
        x_refs, refs = refs[:count], refs[count:]
        s_refs, refs = refs[: count * n_shaped], refs[count * n_shaped :]
        p_refs, refs = refs[:count], refs[count:]
        if first is not None:
            init, refs = refs[0], refs[1:]
        outs, acc = refs[: len(out_shape)], refs[len(out_shape)]
        step = pl.program_id(0)

        @pl.when(step == 0)
        def _():
            acc[...] = jnp.zeros_like(acc) if first is None else init[...]

        for w in range(n_shaped):
            for m in range(2):
                low = (2 * w + m) * half
                total = acc[:, low : low + half]
                for x_ref, s_ref in zip(x_refs, s_refs[w * count : (w + 1) * count]):
                    total = total + jnp.dot(x_ref[...], s_ref[m], preferred_element_type=F32)
                acc[:, low : low + half] = total
        low = 2 * half * n_shaped
        total = acc[:, low:]
        for x_ref, p_ref in zip(x_refs, p_refs):
            total = total + jnp.dot(x_ref[...], p_ref[...], preferred_element_type=F32)
        acc[:, low:] = total

        @pl.when(step == steps - 1)
        def _():
            if first is None:
                outs[0][...] = acc[...]
            elif not shaped:
                outs[0][...] = acc[...].astype(BF16)
            else:
                hold = refs[-1]
                lead = scalars[count]
                for h in range(heads):
                    key, query = (
                        [acc[:, (2 * w + m) * half + h * HEAD_DIM : (2 * w + m) * half + (h + 1) * HEAD_DIM] for m in range(2)]
                        for w in range(2)
                    )
                    value = [acc[:, low + h * pair : low + (h + 1) * pair]]
                    hold[h ^ lead] = jnp.concatenate(key + value + query, axis=1).astype(BF16)
                for j in range(heads):
                    outs[j][...] = hold[j]
                    outs[heads + j][...] = hold[j, :, : 2 * pair]

    def w_shaped(i):
        return pl.BlockSpec((2, sub, half), lambda k, sc: (0, sc[i] * steps + k, 0))

    def w_plain(i):
        return pl.BlockSpec((sub, wide), lambda k, sc: (sc[i] * steps + k, 0))

    in_specs = [pl.BlockSpec((rows, sub), lambda k, sc: (0, k)) for _ in range(count)]
    in_specs += [w_shaped(i) for _ in shaped for i in range(count)] + [w_plain(i) for i in range(count)]
    args = list(pieces) + [w for w in shaped for _ in range(count)] + [plain] * count
    scratch = [pltpu.VMEM(acc_shape.shape, F32)]
    if first is not None:
        in_specs.append(pl.BlockSpec(acc_shape.shape, lambda k, sc: (0, 0)))
        args.append(first)
    if first is None:
        out_shape = [acc_shape]
    elif not shaped:
        out_shape = [jax.ShapeDtypeStruct((rows, wide), BF16)]
    else:
        out_shape = [jax.ShapeDtypeStruct((rows, 3 * pair), BF16)] * heads
        out_shape += [jax.ShapeDtypeStruct((rows, 2 * pair), BF16)] * heads
        scratch.append(pltpu.VMEM((heads, rows, 3 * pair), BF16))
    out_specs = [pl.BlockSpec(o.shape, lambda k, sc: (0, 0)) for o in out_shape]
    scalars = jnp.stack([b.astype(jnp.int32) for b in blocks] + [rank.astype(jnp.int32)])
    flops = 2 * rows * depth * count * acc_shape.shape[1]
    return pl.pallas_call(
        body,
        grid_spec=pltpu.PrefetchScalarGridSpec(
            num_scalar_prefetch=1, grid=(steps,), in_specs=in_specs, out_specs=out_specs, scratch_shapes=scratch
        ),
        out_shape=out_shape,
        cost_estimate=pl.CostEstimate(flops=flops, bytes_accessed=8 << 20, transcendentals=0),
        compiler_params=pltpu.CompilerParams(vmem_limit_bytes=56 * 2**20),
        name="project",
    )(scalars, *args)


def attend(q, kv, state, lam, gain):
    blocks, rows, width = q.shape
    count = len(kv)
    last = state is not None
    lanes = 2 * HEAD_DIM
    extra = log_rows(rows)

    def body(*refs):
        lam_ref, gain_ref, q_ref, refs = refs[0], refs[1], refs[2], refs[3:]
        kv_refs, refs = refs[:count], refs[count:]
        if last:
            acc_in, max_in, attn_ref = refs
        else:
            acc_out, max_out = refs
        query = q_ref[0] * jnp.asarray(HEAD_DIM ** (-0.5), BF16)
        lane = lax.broadcasted_iota(jnp.int32, (rows, width), 1)
        ones = jnp.ones((kv_refs[0].shape[0], 2 * HEAD_DIM), BF16)
        maps, terms = [], []
        for m in range(2):
            mine = (lane // HEAD_DIM) == m
            query_m = jnp.where(mine, query, jnp.zeros_like(query))
            scores = [
                lax.dot_general(
                    query_m, r[:, : 2 * HEAD_DIM], (((1,), (1,)), ((), ())), preferred_element_type=F32
                )
                for r in kv_refs
            ]
            top = scores[0]
            for s in scores[1:]:
                top = jnp.maximum(top, s)
            top = jnp.max(top, axis=1, keepdims=True)
            if last:
                old = max_in[0, m][:, :1]
                top = jnp.maximum(top, old)
                total = acc_in[0, m] * jnp.exp(old - top)
            else:
                total = None
            for s, r in zip(scores, kv_refs):
                expo = jnp.exp(s - top).astype(BF16)
                side = jnp.concatenate([r[:, 2 * HEAD_DIM : 4 * HEAD_DIM], ones], axis=1)
                add = jnp.dot(expo, side, preferred_element_type=F32)
                total = add if total is None else total + add
            if not last:
                acc_out[0, m] = total
                max_out[0, m] = jnp.broadcast_to(top, (rows, 2 * HEAD_DIM))
            else:
                sums = total[:, 2 * HEAD_DIM :]
                maps.append(total[:, : 2 * HEAD_DIM] / sums)
                logs = jnp.transpose(top + jnp.log(sums))[:1]
                for _ in range(LOG_TERMS):
                    term = logs.astype(BF16)
                    logs = logs - term.astype(F32)
                    terms += [term[:, i : i + lanes].astype(F32) for i in range(0, rows, lanes)]
        if last:
            diff = maps[0] - lam_ref[0] * maps[1]
            norm = lax.rsqrt(jnp.mean(diff * diff, axis=1, keepdims=True) + 1e-05)
            attn_ref[0, :rows] = (diff * norm * gain_ref[...]).astype(BF16)
            terms.append(jnp.zeros((extra - len(terms), lanes), F32))
            attn_ref[0, rows:] = jnp.concatenate(terms, axis=0).astype(BF16)

    whole = 4 * HEAD_DIM
    in_specs = [
        pl.BlockSpec(memory_space=pltpu.SMEM),
        pl.BlockSpec((1, gain.shape[1]), lambda b: (0, 0)),
        pl.BlockSpec((1, rows, width), lambda b: (b, 0, 0)),
    ] + [pl.BlockSpec(a.shape, lambda b: (0, 0)) for a in kv]
    acc_spec = pl.BlockSpec((1, 2, rows, whole), lambda b: (b, 0, 0, 0))
    max_spec = pl.BlockSpec((1, 2, rows, 2 * HEAD_DIM), lambda b: (b, 0, 0, 0))
    args = [lam, gain, q, *kv]
    if last:
        in_specs += [acc_spec, max_spec]
        args += list(state)
        out_shape = [
            jax.ShapeDtypeStruct((blocks, rows + extra, 2 * HEAD_DIM), BF16),
        ]
        out_specs = [
            pl.BlockSpec((1, rows + extra, 2 * HEAD_DIM), lambda b: (b, 0, 0)),
        ]
    else:
        out_shape = [
            jax.ShapeDtypeStruct((blocks, 2, rows, whole), F32),
            jax.ShapeDtypeStruct((blocks, 2, rows, 2 * HEAD_DIM), F32),
        ]
        out_specs = [acc_spec, max_spec]
    pairs = 2 * blocks * rows * count * kv[0].shape[0]
    return pl.pallas_call(
        body,
        grid=(blocks,),
        in_specs=in_specs,
        out_specs=out_specs,
        out_shape=out_shape,
        cost_estimate=pl.CostEstimate(flops=pairs * 12 * HEAD_DIM, bytes_accessed=8 << 20, transcendentals=pairs),
        compiler_params=pltpu.CompilerParams(vmem_limit_bytes=56 * 2**20),
        name="attend",
    )(*args)


def pool(pool_in, before, after):
    tok_rows, channels = pool_in.shape
    padded = jnp.concatenate([before, pool_in, after], axis=0).astype(F32)
    total_tok = tok_rows * lax.axis_size("sp")
    position = lax.axis_index("sp") * tok_rows + jnp.arange(tok_rows, dtype=jnp.int32)
    group = (lax.axis_index("tp") * channels + jnp.arange(channels, dtype=jnp.int32)) // (POOL_WIDTH // 4)
    result = jnp.zeros((tok_rows, channels), F32)
    for group_index, reach in enumerate((2, 4, 8, 16)):
        radius = reach // 2
        window_sum = padded[8 - radius : 8 - radius + tok_rows]
        for shift_by in range(-radius + 1, radius):
            window_sum = window_sum + padded[8 + shift_by : 8 + shift_by + tok_rows]
        low = jnp.clip(position - radius, 0, total_tok)
        high = jnp.clip(position + radius, 0, total_tok)
        window_mean = window_sum / (high - low).astype(F32)[:, None]
        result = jnp.where((group == group_index)[None, :], window_mean, result)
    return (result - pool_in.astype(F32)).astype(BF16)


def on_device(
    inputs,
    query_weight,
    key_weight,
    value_weight,
    pool_weight,
    mix_lambda,
    head_gain,
    attn_out_weight,
    pool_out_weight,
):
    tok_rows = inputs.shape[0]
    heads = query_weight.shape[2] // HEAD_DIM
    n_sp, n_tp = lax.axis_size("sp"), lax.axis_size("tp")
    sp, tp = lax.axis_index("sp"), lax.axis_index("tp")
    rank = sp % heads

    pieces = {0: inputs}
    for offset in range(2, n_tp, 2):
        pieces[offset] = swap(inputs, "tp", offset)
    pieces[1] = swap(inputs, "tp", 1)
    near, far = [0, 1], list(range(2, n_tp))
    place = lambda which: ([pieces[d] for d in which], [tp ^ d for d in which])
    shaped = (key_weight, query_weight)
    (main_sum,) = project(*place(near), shaped, value_weight, None, rank)
    (pool_sum,) = project(*place(near), (), pool_weight, None, rank)
    for offset in range(2, n_tp, 2):
        pieces[offset + 1] = swap(pieces[offset], "tp", 1)
    made = project(*place(far), shaped, value_weight, main_sum, rank)

    own, rest = made[:heads], made[heads:]
    parts = [own[0]] + [swap(own[d], "sp", d) for d in range(1, heads)]
    parts += [swap(rest[d % heads], "sp", d) for d in range(heads, n_sp)]
    (pool_in,) = project(*place(far), (), pool_weight, pool_sum, rank)
    up = [(i, i + 1) for i in range(n_sp - 1)]
    before = lax.ppermute(pool_in[tok_rows - 8 :], "sp", up)
    after = lax.ppermute(pool_in[:8], "sp", [(j, i) for i, j in up])
    pooled = pool(pool_in, before, after)

    lam = lax.dynamic_slice(mix_lambda, (rank,), (1,))
    gain = head_gain[None, :]
    queries = jnp.stack([part[:, 4 * HEAD_DIM :] for part in parts[:heads]])
    state = attend(queries, parts[: n_sp // 2], None, lam, gain)
    (attn,) = attend(queries, parts[n_sp // 2 :], state, lam, gain)

    mine = jnp.zeros((tok_rows, heads * 2 * HEAD_DIM), BF16)
    log_totals = jnp.zeros((2, heads, tok_rows), F32)
    for d in range(heads):
        part = swap(attn[d], "sp", d) if d else attn[d]
        log = part[tok_rows:].reshape(-1)[: 2 * LOG_TERMS * tok_rows].reshape(2, LOG_TERMS, tok_rows)
        log = sum(log[:, i].astype(F32) for i in range(LOG_TERMS))
        mine = lax.dynamic_update_slice(mine, part[:tok_rows], (0, (rank ^ d) * 2 * HEAD_DIM))
        log_totals = lax.dynamic_update_slice(log_totals, log[:, None, :], (0, rank ^ d, 0))

    chip_rows = 2 * tok_rows // n_tp

    def partial(e):
        at = ((tp ^ e) // 2) * chip_rows
        a = lax.dynamic_slice(mine, (at, 0), (chip_rows, mine.shape[1]))
        p = lax.dynamic_slice(pooled, (at, 0), (chip_rows, pooled.shape[1]))
        both = (
            jnp.dot(a, attn_out_weight, preferred_element_type=F32)
            + jnp.dot(p, pool_out_weight, preferred_element_type=F32)
        ).astype(BF16)
        both = lax.optimization_barrier(both.reshape(2, chip_rows // 2, both.shape[1]))
        return (
            lax.dynamic_index_in_dim(both, tp % 2, 0, keepdims=False),
            lax.dynamic_index_in_dim(both, 1 - tp % 2, 0, keepdims=False),
        )

    total = None
    for e in list(range(2, n_tp, 2)) + [0]:
        kept, sent = partial(e)
        pair = kept.astype(F32) + swap(sent, "tp", 1).astype(F32)
        if e:
            pair = swap(pair.astype(BF16), "tp", e).astype(F32)
        total = pair if total is None else total + pair
    return (total.astype(BF16), log_totals)


def solution(mesh):
    in_specs = (
        P("sp", "tp"),
        P(None, None, "tp"),
        P(None, None, "tp"),
        P(None, "tp"),
        P(None, "tp"),
        P("tp"),
        P(),
        P("tp", None),
        P("tp", None),
    )
    out_specs = (P(("sp", "tp"), None), P(None, "tp", "sp"))

    return jax.shard_map(on_device, mesh=mesh, in_specs=in_specs, out_specs=out_specs, check_vma=False)
```

```python
import jax
import jax.numpy as jnp
from jax import lax
from jax.experimental import pallas as pl
from jax.experimental.pallas import tpu as pltpu
from jax.sharding import PartitionSpec as P


HEAD_DIM = 64
POOL_WIDTH = 2048
F32 = jnp.float32
BF16 = jnp.bfloat16


LOG_TERMS = 3


def log_rows(rows):
    return -(-2 * LOG_TERMS * rows // (2 * HEAD_DIM) // 16) * 16


def swap(value, axis, offset):
    count = lax.axis_size(axis)
    return lax.ppermute(value, axis, [(i, i ^ offset) for i in range(count)])


def project(pieces, blocks, shaped, plain, first, rank):
    rows, depth = pieces[0].shape
    count, n_shaped = len(pieces), len(shaped)
    half = shaped[0].shape[2] if shaped else 0
    heads = half // HEAD_DIM
    wide = plain.shape[1]
    steps = 2
    sub = depth // steps
    pair = 2 * HEAD_DIM
    acc_shape = jax.ShapeDtypeStruct((rows, 2 * half * n_shaped + wide), F32)

    def body(scalars, *refs):
        x_refs, refs = refs[:count], refs[count:]
        s_refs, refs = refs[: count * n_shaped], refs[count * n_shaped :]
        p_refs, refs = refs[:count], refs[count:]
        if first is not None:
            init, refs = refs[0], refs[1:]
        outs, acc = refs[: len(out_shape)], refs[len(out_shape)]
        step = pl.program_id(0)

        @pl.when(step == 0)
        def _():
            acc[...] = jnp.zeros_like(acc) if first is None else init[...]

        for w in range(n_shaped):
            for m in range(2):
                low = (2 * w + m) * half
                total = acc[:, low : low + half]
                for x_ref, s_ref in zip(x_refs, s_refs[w * count : (w + 1) * count]):
                    total = total + jnp.dot(x_ref[...], s_ref[m], preferred_element_type=F32)
                acc[:, low : low + half] = total
        low = 2 * half * n_shaped
        total = acc[:, low:]
        for x_ref, p_ref in zip(x_refs, p_refs):
            total = total + jnp.dot(x_ref[...], p_ref[...], preferred_element_type=F32)
        acc[:, low:] = total

        @pl.when(step == steps - 1)
        def _():
            if first is None:
                outs[0][...] = acc[...]
            elif not shaped:
                outs[0][...] = acc[...].astype(BF16)
            else:
                hold = refs[-1]
                lead = scalars[count]
                for h in range(heads):
                    key, query = (
                        [acc[:, (2 * w + m) * half + h * HEAD_DIM : (2 * w + m) * half + (h + 1) * HEAD_DIM] for m in range(2)]
                        for w in range(2)
                    )
                    value = [acc[:, low + h * pair : low + (h + 1) * pair]]
                    hold[h ^ lead] = jnp.concatenate(key + value + query, axis=1).astype(BF16)
                for j in range(heads):
                    outs[j][...] = hold[j]
                    outs[heads + j][...] = hold[j, :, : 2 * pair]

    def w_shaped(i):
        return pl.BlockSpec((2, sub, half), lambda k, sc: (0, sc[i] * steps + k, 0))

    def w_plain(i):
        return pl.BlockSpec((sub, wide), lambda k, sc: (sc[i] * steps + k, 0))

    in_specs = [pl.BlockSpec((rows, sub), lambda k, sc: (0, k)) for _ in range(count)]
    in_specs += [w_shaped(i) for _ in shaped for i in range(count)] + [w_plain(i) for i in range(count)]
    args = list(pieces) + [w for w in shaped for _ in range(count)] + [plain] * count
    scratch = [pltpu.VMEM(acc_shape.shape, F32)]
    if first is not None:
        in_specs.append(pl.BlockSpec(acc_shape.shape, lambda k, sc: (0, 0)))
        args.append(first)
    if first is None:
        out_shape = [acc_shape]
    elif not shaped:
        out_shape = [jax.ShapeDtypeStruct((rows, wide), BF16)]
    else:
        out_shape = [jax.ShapeDtypeStruct((rows, 3 * pair), BF16)] * heads
        out_shape += [jax.ShapeDtypeStruct((rows, 2 * pair), BF16)] * heads
        scratch.append(pltpu.VMEM((heads, rows, 3 * pair), BF16))
    out_specs = [pl.BlockSpec(o.shape, lambda k, sc: (0, 0)) for o in out_shape]
    scalars = jnp.stack([b.astype(jnp.int32) for b in blocks] + [rank.astype(jnp.int32)])
    flops = 2 * rows * depth * count * acc_shape.shape[1]
    return pl.pallas_call(
        body,
        grid_spec=pltpu.PrefetchScalarGridSpec(
            num_scalar_prefetch=1, grid=(steps,), in_specs=in_specs, out_specs=out_specs, scratch_shapes=scratch
        ),
        out_shape=out_shape,
        cost_estimate=pl.CostEstimate(flops=flops, bytes_accessed=8 << 20, transcendentals=0),
        compiler_params=pltpu.CompilerParams(vmem_limit_bytes=56 * 2**20),
        name="project",
    )(scalars, *args)


def attend(q, kv, state, lam, gain):
    blocks, rows, width = q.shape
    count = len(kv)
    last = state is not None
    lanes = 2 * HEAD_DIM
    extra = log_rows(rows)

    def body(*refs):
        lam_ref, gain_ref, q_ref, refs = refs[0], refs[1], refs[2], refs[3:]
        kv_refs, refs = refs[:count], refs[count:]
        if last:
            acc_in, max_in, attn_ref = refs
        else:
            acc_out, max_out = refs
        query = q_ref[0] * jnp.asarray(HEAD_DIM ** (-0.5), BF16)
        lane = lax.broadcasted_iota(jnp.int32, (rows, width), 1)
        keys = jnp.concatenate([r[:, : 2 * HEAD_DIM] for r in kv_refs], axis=0)
        side = jnp.concatenate([r[:, 2 * HEAD_DIM : 4 * HEAD_DIM] for r in kv_refs], axis=0)
        side = jnp.concatenate([side, jnp.ones_like(side)], axis=1)
        maps, terms = [], []
        for m in range(2):
            mine = (lane // HEAD_DIM) == m
            query_m = jnp.where(mine, query, jnp.zeros_like(query))
            scores = lax.dot_general(
                query_m, keys, (((1,), (1,)), ((), ())), preferred_element_type=F32
            )
            top = jnp.max(scores, axis=1, keepdims=True)
            if last:
                old = max_in[0, m][:, :1]
                top = jnp.maximum(top, old)
            expo = jnp.exp(scores - top).astype(BF16)
            total = jnp.dot(expo, side, preferred_element_type=F32)
            if last:
                total = total + acc_in[0, m] * jnp.exp(old - top)
            if not last:
                acc_out[0, m] = total
                max_out[0, m] = jnp.broadcast_to(top, (rows, 2 * HEAD_DIM))
            else:
                sums = total[:, 2 * HEAD_DIM :]
                maps.append(total[:, : 2 * HEAD_DIM] / sums)
                logs = jnp.transpose(top + jnp.log(sums))[:1]
                for _ in range(LOG_TERMS):
                    term = logs.astype(BF16)
                    logs = logs - term.astype(F32)
                    terms += [term[:, i : i + lanes].astype(F32) for i in range(0, rows, lanes)]
        if last:
            diff = maps[0] - lam_ref[0] * maps[1]
            norm = lax.rsqrt(jnp.mean(diff * diff, axis=1, keepdims=True) + 1e-05)
            attn_ref[0, :rows] = (diff * norm * gain_ref[...]).astype(BF16)
            terms.append(jnp.zeros((extra - len(terms), lanes), F32))
            attn_ref[0, rows:] = jnp.concatenate(terms, axis=0).astype(BF16)

    whole = 4 * HEAD_DIM
    in_specs = [
        pl.BlockSpec(memory_space=pltpu.SMEM),
        pl.BlockSpec((1, gain.shape[1]), lambda b: (0, 0)),
        pl.BlockSpec((1, rows, width), lambda b: (b, 0, 0)),
    ] + [pl.BlockSpec(a.shape, lambda b: (0, 0)) for a in kv]
    acc_spec = pl.BlockSpec((1, 2, rows, whole), lambda b: (b, 0, 0, 0))
    max_spec = pl.BlockSpec((1, 2, rows, 2 * HEAD_DIM), lambda b: (b, 0, 0, 0))
    args = [lam, gain, q, *kv]
    if last:
        in_specs += [acc_spec, max_spec]
        args += list(state)
        out_shape = [
            jax.ShapeDtypeStruct((blocks, rows + extra, 2 * HEAD_DIM), BF16),
        ]
        out_specs = [
            pl.BlockSpec((1, rows + extra, 2 * HEAD_DIM), lambda b: (b, 0, 0)),
        ]
    else:
        out_shape = [
            jax.ShapeDtypeStruct((blocks, 2, rows, whole), F32),
            jax.ShapeDtypeStruct((blocks, 2, rows, 2 * HEAD_DIM), F32),
        ]
        out_specs = [acc_spec, max_spec]
    pairs = 2 * blocks * rows * count * kv[0].shape[0]
    return pl.pallas_call(
        body,
        grid=(blocks,),
        in_specs=in_specs,
        out_specs=out_specs,
        out_shape=out_shape,
        cost_estimate=pl.CostEstimate(flops=pairs * 12 * HEAD_DIM, bytes_accessed=8 << 20, transcendentals=pairs),
        compiler_params=pltpu.CompilerParams(vmem_limit_bytes=56 * 2**20),
        name="attend",
    )(*args)


def pool(pool_in, before, after):
    tok_rows, channels = pool_in.shape
    padded = jnp.concatenate([before, pool_in, after], axis=0).astype(F32)
    total_tok = tok_rows * lax.axis_size("sp")
    position = lax.axis_index("sp") * tok_rows + jnp.arange(tok_rows, dtype=jnp.int32)
    group = (lax.axis_index("tp") * channels + jnp.arange(channels, dtype=jnp.int32)) // (POOL_WIDTH // 4)
    result = jnp.zeros((tok_rows, channels), F32)
    for group_index, reach in enumerate((2, 4, 8, 16)):
        radius = reach // 2
        window_sum = padded[8 - radius : 8 - radius + tok_rows]
        for shift_by in range(-radius + 1, radius):
            window_sum = window_sum + padded[8 + shift_by : 8 + shift_by + tok_rows]
        low = jnp.clip(position - radius, 0, total_tok)
        high = jnp.clip(position + radius, 0, total_tok)
        window_mean = window_sum / (high - low).astype(F32)[:, None]
        result = jnp.where((group == group_index)[None, :], window_mean, result)
    return (result - pool_in.astype(F32)).astype(BF16)


def on_device(
    inputs,
    query_weight,
    key_weight,
    value_weight,
    pool_weight,
    mix_lambda,
    head_gain,
    attn_out_weight,
    pool_out_weight,
):
    tok_rows = inputs.shape[0]
    heads = query_weight.shape[2] // HEAD_DIM
    n_sp, n_tp = lax.axis_size("sp"), lax.axis_size("tp")
    sp, tp = lax.axis_index("sp"), lax.axis_index("tp")
    rank = sp % heads

    pieces = {0: inputs}
    for offset in range(2, n_tp, 2):
        pieces[offset] = swap(inputs, "tp", offset)
    pieces[1] = swap(inputs, "tp", 1)
    near, far = [0, 1], list(range(2, n_tp))
    place = lambda which: ([pieces[d] for d in which], [tp ^ d for d in which])
    shaped = (key_weight, query_weight)
    (main_sum,) = project(*place(near), shaped, value_weight, None, rank)
    (pool_sum,) = project(*place(near), (), pool_weight, None, rank)
    for offset in range(2, n_tp, 2):
        pieces[offset + 1] = swap(pieces[offset], "tp", 1)
    made = project(*place(far), shaped, value_weight, main_sum, rank)

    own, rest = made[:heads], made[heads:]
    parts = [own[0]] + [swap(own[d], "sp", d) for d in range(1, heads)]
    parts += [swap(rest[d % heads], "sp", d) for d in range(heads, n_sp)]
    (pool_in,) = project(*place(far), (), pool_weight, pool_sum, rank)
    up = [(i, i + 1) for i in range(n_sp - 1)]
    before = lax.ppermute(pool_in[tok_rows - 8 :], "sp", up)
    after = lax.ppermute(pool_in[:8], "sp", [(j, i) for i, j in up])
    pooled = pool(pool_in, before, after)

    lam = lax.dynamic_slice(mix_lambda, (rank,), (1,))
    gain = head_gain[None, :]
    queries = jnp.stack([part[:, 4 * HEAD_DIM :] for part in parts[:heads]])
    state = attend(queries, parts[: n_sp // 2], None, lam, gain)
    (attn,) = attend(queries, parts[n_sp // 2 :], state, lam, gain)

    mine = jnp.zeros((tok_rows, heads * 2 * HEAD_DIM), BF16)
    log_totals = jnp.zeros((2, heads, tok_rows), F32)
    for d in range(heads):
        part = swap(attn[d], "sp", d) if d else attn[d]
        log = part[tok_rows:].reshape(-1)[: 2 * LOG_TERMS * tok_rows].reshape(2, LOG_TERMS, tok_rows)
        log = sum(log[:, i].astype(F32) for i in range(LOG_TERMS))
        mine = lax.dynamic_update_slice(mine, part[:tok_rows], (0, (rank ^ d) * 2 * HEAD_DIM))
        log_totals = lax.dynamic_update_slice(log_totals, log[:, None, :], (0, rank ^ d, 0))

    chip_rows = 2 * tok_rows // n_tp

    def partial(e):
        at = ((tp ^ e) // 2) * chip_rows
        a = lax.dynamic_slice(mine, (at, 0), (chip_rows, mine.shape[1]))
        p = lax.dynamic_slice(pooled, (at, 0), (chip_rows, pooled.shape[1]))
        both = (
            jnp.dot(a, attn_out_weight, preferred_element_type=F32)
            + jnp.dot(p, pool_out_weight, preferred_element_type=F32)
        ).astype(BF16)
        both = lax.optimization_barrier(both.reshape(2, chip_rows // 2, both.shape[1]))
        return (
            lax.dynamic_index_in_dim(both, tp % 2, 0, keepdims=False),
            lax.dynamic_index_in_dim(both, 1 - tp % 2, 0, keepdims=False),
        )

    total = None
    for e in list(range(2, n_tp, 2)) + [0]:
        kept, sent = partial(e)
        pair = kept.astype(F32) + swap(sent, "tp", 1).astype(F32)
        if e:
            pair = swap(pair.astype(BF16), "tp", e).astype(F32)
        total = pair if total is None else total + pair
    return (total.astype(BF16), log_totals)


def solution(mesh):
    in_specs = (
        P("sp", "tp"),
        P(None, None, "tp"),
        P(None, None, "tp"),
        P(None, "tp"),
        P(None, "tp"),
        P("tp"),
        P(),
        P("tp", None),
        P("tp", None),
    )
    out_specs = (P(("sp", "tp"), None), P(None, "tp", "sp"))

    return jax.shard_map(on_device, mesh=mesh, in_specs=in_specs, out_specs=out_specs, check_vma=False)
```
